512 devices in a mesh: rep: 2 (over z_hi), fs: 32 (over z_lo, y), tp: 8 (over x, core).
Axes of the slice: x: 4, y: 4, z: 16 (z_hi: 2, z_lo: 8; z = z_hi * 8 + z_lo), core: 2. Of those that a mesh axis runs over, the one named last changes fastest.
Arguments:
- stream: bfloat16 [16384, 2048], P(('rep', 'fs'), 'tp'), may hold values from -6 to 6
- norm_gains: float32 [6, 2048], replicated, may hold values from 0.1 to 1.9
- w_gate: bfloat16 [2048, 5632], P('fs', 'tp'), may hold values from -0.125 to 0.125
- w_up: bfloat16 [2048, 5632], P('fs', 'tp'), may hold values from -0.125 to 0.125
- w_down: bfloat16 [5632, 2048], P('tp', 'fs'), may hold values from -0.15625 to 0.15625
- w_inner: bfloat16 [2048, 1024], P('fs', 'tp'), may hold values from -0.125 to 0.125
- w_bgate: bfloat16 [2048, 1024], P('fs', 'tp'), may hold values from -0.125 to 0.125
- w_cgate: bfloat16 [2048, 1024], P('fs', 'tp'), may hold values from -0.125 to 0.125
- conv_taps: float32 [3, 1024], P(None, 'tp'), may hold values from -3.5 to 3.5
- w_out: bfloat16 [1024, 2048], P('tp', 'fs'), may hold values from -0.375 to 0.375
Outputs:
- mixed: bfloat16 [16384, 2048], P(('rep', 'fs'), 'tp')
The draws below stay inside these ranges and needn't reach their ends.
All inputs are finite; a program needn't handle non-finite values.
Results may differ from the reference program's by a relative error of at most 0.02.
Values may be sent and summed in bfloat16 or wider, within the bound.
A program may use at most 64 MiB of HBM per device.

```python
import jax
import jax.numpy as jnp
from jax import lax

D = 2048
FF = 5632
CW = 1024
TAPS = 3
SEQ_LEN = 8192
TOKENS = 16384
N_TP = 8


def strengthened(values, rng, source, target, shards_of, factor):
    def block_of(position):
        return (jnp.arange(values.shape[position]) // (values.shape[position] // shards_of)).reshape((-1,) + (1,) * (values.ndim - 1 - position))

    one_side = jax.random.permutation(rng, shards_of)[block_of(target)]
    second = (block_of(target) + shards_of // 2) % shards_of
    return jnp.where((block_of(source) == one_side) | (block_of(source) == second), factor * values, values)


def levels(key, extent, pieces, least, largest):
    level, own = 1.0, jax.random.fold_in(key, 6)
    for dim, blocks in pieces:
        draws = jnp.exp(jax.random.uniform(jax.random.fold_in(own, dim), (blocks,), jnp.float32, least / len(pieces), largest / len(pieces)))
        level = level * jnp.repeat(draws, extent[dim] // blocks).reshape([-1 if axis == dim else 1 for axis in range(len(extent))])
    return level


def normal_values(rng, dims, width, limit, cuts=(), held_as=jnp.bfloat16):
    array = jax.random.normal(rng, dims, jnp.float32) * width
    if len(cuts) > 0:
        array = levels(rng, dims, cuts, -0.22, 0.18) * array
    return jnp.clip(array, min=-limit, max=limit).astype(held_as)


def noise_with(rng, extent, deviation, most, shards, heavy, dtype=jnp.bfloat16):
    values = deviation * jax.random.normal(rng, extent, jnp.float32)
    if shards:
        values = values * levels(rng, extent, shards, -0.22, 0.18)
    return jnp.clip(strengthened(values, jax.random.fold_in(rng, 3), *heavy), -most, most).astype(dtype)


def setup_inputs(seed: int = 0) -> dict:
    key_list = jax.random.split(jax.random.key(seed), 11)
    return {
        "stream": normal_values(key_list[0], (TOKENS, D), 1.0, 6.0, ((0, 64), (1, 8))),
        "norm_gains": jnp.clip(1.0 + 0.18 * jax.random.normal(key_list[1], (6, D), jnp.float32), 0.1, 1.9),
        "w_gate": normal_values(key_list[2], (D, FF), D ** -0.5, 0.125, ((0, 32), (1, 8))),
        "w_up": normal_values(key_list[3], (D, FF), D ** -0.5, 0.125, ((0, 32), (1, 8))),
        "w_down": noise_with(key_list[4], (FF, D), FF ** -0.5, 0.15625, ((0, 8), (1, 32)), (0, 1, 32, 2.75)),
        "w_inner": normal_values(key_list[5], (D, CW), D ** -0.5, 0.125, ((0, 32), (1, 8))),
        "w_bgate": normal_values(key_list[6], (D, CW), D ** -0.5, 0.125, ((0, 32), (1, 8))),
        "w_cgate": normal_values(key_list[7], (D, CW), D ** -0.5, 0.125, ((0, 32), (1, 8))),
        "conv_taps": normal_values(key_list[8], (TAPS, CW), TAPS ** -0.5, 3.5, ((1, 8),), jnp.float32),
        "w_out": noise_with(key_list[9], (CW, D), CW ** -0.5, 0.375, ((0, 8), (1, 32)), (0, 1, 32, 2.75)),
    }


EPSILON = 1e-06

def rms_scale(values):
    return values * lax.rsqrt(lax.optimization_barrier(jnp.mean(values * values, axis=1, keepdims=True)) + EPSILON)

def norm_input(current, gain):
    return (rms_scale(current.astype(jnp.float32)) * gain).astype(jnp.bfloat16)

def split_sum(hidden, weight, groups):
    columns = hidden.shape[1] // groups
    result = jnp.zeros((hidden.shape[0], weight.shape[1]), jnp.float32)
    for group in range(groups):
        partial_term = jnp.dot(hidden[:, group * columns:(group + 1) * columns], weight[group * columns:(group + 1) * columns], preferred_element_type=jnp.float32)
        rounded = lax.optimization_barrier(partial_term.astype(jnp.bfloat16))
        result = result + rounded.astype(jnp.float32)
    return result

def settle(current, branch_sum, gain, weight):
    return (current.astype(jnp.float32) + weight * (rms_scale(branch_sum) * gain)).astype(jnp.bfloat16)

def feed_forward(current, gain_in, gain_out, w_gate, w_up, w_down):
    normed = norm_input(current, gain_in)
    gate_vals = jnp.dot(normed, w_gate, preferred_element_type=jnp.float32)
    upward = jnp.dot(normed, w_up, preferred_element_type=jnp.float32)
    hidden = (jax.nn.silu(gate_vals) * upward).astype(jnp.bfloat16)
    return settle(current, split_sum(hidden, w_down, N_TP), gain_out, 0.5)

def reference(stream, norm_gains, w_gate, w_up, w_down, w_inner, w_bgate, w_cgate, conv_taps, w_out):
    first = feed_forward(stream, norm_gains[0], norm_gains[1], w_gate, w_up, w_down)
    normed = norm_input(first, norm_gains[2])
    inner = jnp.dot(normed, w_inner, preferred_element_type=jnp.float32)
    bgate = jnp.dot(normed, w_bgate, preferred_element_type=jnp.float32)
    cgate = jnp.dot(normed, w_cgate, preferred_element_type=jnp.float32)
    conv_input = (cgate * inner).reshape(-1, SEQ_LEN, CW)
    padded = jnp.pad(conv_input, ((0, 0), (TAPS - 1, 0), (0, 0)))
    conv = conv_taps[0] * padded[:, 0:SEQ_LEN]
    for tap in range(1, TAPS):
        conv = conv + conv_taps[tap] * padded[:, tap:tap + SEQ_LEN]
    gated = (bgate * conv.reshape(-1, CW)).astype(jnp.bfloat16)
    second = settle(first, split_sum(gated, w_out, N_TP), norm_gains[3], 1.0)
    return feed_forward(second, norm_gains[4], norm_gains[5], w_gate, w_up, w_down)
```

```python
import jax
import jax.numpy as jnp
from jax import lax
from jax.experimental import pallas as pl
from jax.experimental.pallas import tpu as pltpu
from jax.sharding import PartitionSpec as P

TAPS = 3
EPSILON = 1e-06
Z_LO, Z_ALL, Y = 8, 16, 4
ROWS = 64
PARTS = (
    ((0, 640, "y"), (640, 768, "z")),
    ((0, 256, "y"), (256, 512, "z")),
    ((0, 128, "y"), (128, 384, "z")),
)
WIDTHS = (1408, 768, 512)
RATE = 46.6e3
HOP = 2.0
AHEAD = 4.0


class Copy:
    def __init__(self, number, part, link, dz, dy, row, rows, after):
        self.number, self.part, self.link = number, part, link
        self.dz, self.dy, self.row, self.rows = dz, dy, row, rows
        self.after, self.tail = after, 0.0
        stream, index = part
        self.time = rows * PARTS[stream][index][1] * 2 / RATE
        self.start = None


def all_copies():
    copies = []

    def add(part, link, dz, dy, after, row=0, rows=ROWS):
        copies.append(Copy(len(copies), part, link, dz, dy, row, rows, list(after)))
        return copies[-1]

    half = ROWS // 2
    for stream, parts in enumerate(PARTS):
        for index, (_, _, first) in enumerate(parts):
            part = (stream, index)

            def along_z(dy, own):
                came = {0: own}
                for sign, link, row in ((-1, "z+", 0), (1, "z-", half)):
                    previous = own
                    for step in range(3):
                        previous = [add(part, link, sign * step, dy, previous)]
                        came[sign * (step + 1)] = previous
                    last = add(part, link, sign * 3, dy, previous, row, half)
                    came.setdefault(4, []).append(last)
                return came

            def along_y(dz, own):
                up = add(part, "y+", dz, 0, own)
                down = add(part, "y-", dz, 0, own)
                far = [
                    add(part, "y+", dz, -1, [up], 0, half),
                    add(part, "y-", dz, 1, [down], half, half),
                ]
                return {0: own, -1: [up], 1: [down], 2: far}

            if first == "y":
                for dy, got in along_y(0, []).items():
                    along_z(dy, got)
            else:
                for dz, got in along_z(0, []).items():
                    along_y(dz, got)
    for copy in reversed(copies):
        for before in copy.after:
            before.tail = max(before.tail, copy.tail + copy.time + HOP)
    return copies


def planned():
    copies = all_copies()
    free = dict.fromkeys(("y+", "y-", "z+", "z-"), 0.0)
    waiting, flying, here, order, now = list(copies), [], set(), [], 0.0
    while waiting or flying:
        ready = [c for c in waiting if all(b.number in here for b in c.after)]
        ready.sort(key=lambda c: (c.part[0], -c.tail, c.number))
        for copy in ready:
            if free[copy.link] < now + AHEAD:
                free[copy.link] = max(free[copy.link], now) + copy.time
                flying.append((free[copy.link] + HOP, copy.number, copy))
                waiting.remove(copy)
                order.append(("start", copy, now))
        flying.sort(key=lambda f: f[:2])
        now, _, copy = flying.pop(0)
        here.add(copy.number)
        order.append(("wait", copy, now))
    return order, copies


def gather_kernel(order, copies, own0, own1, own2, full0, full1, full2, send_sem, recv_sem):
    own, full = (own0, own1, own2), (full0, full1, full2)
    rep, fs, tp = lax.axis_index("rep"), lax.axis_index("fs"), lax.axis_index("tp")
    z_lo, y = fs // Y, lax.rem(fs, Y)
    z = rep * Z_LO + z_lo

    def at(z_to, y_to):
        return (z_to // Z_LO, lax.rem(z_to, Z_LO) * Y + y_to, tp)

    place = {
        "y+": at(z, lax.rem(y + 1, Y)),
        "y-": at(z, lax.rem(y + Y - 1, Y)),
        "z+": at(lax.rem(z + 1, Z_ALL), y),
        "z-": at(lax.rem(z + Z_ALL - 1, Z_ALL), y),
    }
    barrier = pltpu.get_barrier_semaphore()
    for device in place.values():
        pl.semaphore_signal(barrier, inc=1, device_id=device, device_id_type=pl.DeviceIdType.MESH)
    pl.semaphore_wait(barrier, len(place))

    def remote(copy):
        stream, index = copy.part
        column, width, _ = PARTS[stream][index]
        columns = pl.ds(column, width)
        block = lax.rem(z_lo + copy.dz + Z_LO, Z_LO) * Y + lax.rem(y + copy.dy + Y, Y)
        rows = pl.ds(pl.multiple_of(block * ROWS, ROWS) + copy.row, copy.rows)
        target = full[stream].at[rows, columns]
        source = target
        if copy.dz == 0 and copy.dy == 0:
            source = own[stream].at[pl.ds(copy.row, copy.rows), columns]
        return pltpu.make_async_remote_copy(
            src_ref=source,
            dst_ref=target,
            send_sem=send_sem.at[copy.number],
            recv_sem=recv_sem.at[copy.number],
            device_id=place[copy.link],
            device_id_type=pl.DeviceIdType.MESH,
        )

    mine = pl.ds(pl.multiple_of(fs * ROWS, ROWS), ROWS)
    for stream in range(3):
        full[stream][mine, :] = own[stream][...]
    for kind, copy, _ in order:
        if kind == "start":
            remote(copy).start()
        else:
            remote(copy).wait_recv()
    for copy in copies:
        remote(copy).wait_send()


def gathered_weights(pieces):
    order, copies = planned()

    def kernel(*refs):
        gather_kernel(order, copies, *refs)

    return pl.pallas_call(
        kernel,
        out_shape=[jax.ShapeDtypeStruct((ROWS * Z_LO * Y, w), jnp.bfloat16) for w in WIDTHS],
        in_specs=[pl.BlockSpec(memory_space=pltpu.VMEM)] * 3,
        out_specs=[pl.BlockSpec(memory_space=pltpu.VMEM)] * 3,
        scratch_shapes=[
            pltpu.SemaphoreType.DMA((len(copies),)),
            pltpu.SemaphoreType.DMA((len(copies),)),
        ],
        compiler_params=pltpu.CompilerParams(collective_id=0, has_side_effects=True),
    )(*pieces)


def laid_out(parts, dim):
    shape = list(parts.shape[1:])
    shape[dim] *= parts.shape[0]
    return jnp.moveaxis(parts, 0, dim).reshape(shape)


def from_everyone(x, axis):
    copies = jnp.broadcast_to(x, (lax.axis_size(axis), *x.shape))
    return lax.all_to_all(copies, axis, split_axis=0, concat_axis=0, tiled=True)


def collect(x, axis, dim):
    return laid_out(from_everyone(x, axis), dim)


def cut_along(x, dim, count):
    shape = x.shape
    parts = x.reshape(*shape[:dim], count, shape[dim] // count, *shape[dim + 1 :])
    return jnp.moveaxis(parts, dim, 0)


def sent_and_summed(x, axis, dim):
    parts = cut_along(x, dim, lax.axis_size(axis))
    arrived = lax.all_to_all(parts, axis, split_axis=0, concat_axis=0, tiled=True)
    return arrived.astype(jnp.float32).sum(axis=0)


def taken_together(x, axis):
    everything = from_everyone(x, axis)
    return jnp.sum(everything, axis=0)


def from_behind(x, axis, by):
    count = lax.axis_size(axis)
    pairs = [(i, i + by) for i in range(count) if 0 <= i + by < count]
    return lax.ppermute(x, axis, pairs)


def packed(w_gate, w_up, w_down, w_inner, w_bgate, w_cgate, w_out):
    first = jnp.concatenate([w_gate, w_up], axis=1)
    second = jnp.pad(w_down.T, ((0, 0), (0, 64)))
    third = jnp.concatenate([w_inner, w_bgate, w_cgate, w_out.T], axis=1)
    return first, second, third


def shards(stream, norm_gains, w_gate, w_up, w_down, w_inner, w_bgate, w_cgate, conv_taps, w_out):
    tp_index = lax.axis_index("tp")
    local_width = stream.shape[1]
    model_width = local_width * lax.axis_size("tp")
    units = w_gate.shape[1]
    channels = w_inner.shape[1]

    def own_gain(row):
        return lax.dynamic_slice_in_dim(norm_gains[row], tp_index * local_width, local_width, 0)

    def gathered_norm(current, row):
        gathered = collect(current, "tp", 1)
        values = gathered.astype(jnp.float32)
        scaled = values * lax.rsqrt(jnp.mean(values * values, axis=1, keepdims=True) + EPSILON)
        return (scaled * norm_gains[row]).astype(jnp.bfloat16)

    def settle(current, partials, row, weight):
        branch_sum = sent_and_summed(partials.astype(jnp.bfloat16), "tp", 1)
        squares = taken_together(jnp.sum(branch_sum * branch_sum, axis=1), "tp")
        scaled = branch_sum * lax.rsqrt(squares / model_width + EPSILON)[:, None]
        return (current.astype(jnp.float32) + weight * (scaled * own_gain(row))).astype(
            jnp.bfloat16
        )

    both_whole, down_whole, mix_whole = gathered_weights(
        packed(w_gate, w_up, w_down, w_inner, w_bgate, w_cgate, w_out)
    )

    def onto(x, turned):
        return lax.dot_general(
            x, turned, (((1,), (1,)), ((), ())), preferred_element_type=jnp.float32
        )

    def feed_forward(current, row_in, row_out):
        normed = gathered_norm(current, row_in)
        both = jnp.dot(normed, both_whole, preferred_element_type=jnp.float32)
        gate_vals, upward = both[:, :units], both[:, units:]
        hidden = (jax.nn.silu(gate_vals) * upward).astype(jnp.bfloat16)
        return settle(current, onto(hidden, down_whole[:, :units]), row_out, 0.5)

    first = feed_forward(stream, 0, 1)
    normed_mix = gathered_norm(first, 2)
    local_rows = normed_mix.shape[0]
    mix_in = jnp.dot(normed_mix, mix_whole[:, : 3 * channels], preferred_element_type=jnp.float32)
    inner, bgate, cgate = (mix_in[:, i * channels : (i + 1) * channels] for i in range(3))
    conv_input = cgate * inner
    earlier = from_behind(conv_input[local_rows - (TAPS - 1) :], "fs", 1)
    padded = jnp.concatenate([earlier, conv_input], axis=0)
    conv = conv_taps[0] * padded[0:local_rows]
    for tap in range(1, TAPS):
        conv = conv + conv_taps[tap] * padded[tap : tap + local_rows]
    gated = (bgate * conv).astype(jnp.bfloat16)
    second = settle(first, onto(gated, mix_whole[:, 3 * channels :]), 3, 1.0)
    return feed_forward(second, 4, 5)


def solution(mesh):
    return jax.shard_map(
        shards,
        mesh=mesh,
        in_specs=(
            P(("rep", "fs"), "tp"),
            P(),
            P("fs", "tp"),
            P("fs", "tp"),
            P("tp", "fs"),
            P("fs", "tp"),
            P("fs", "tp"),
            P("fs", "tp"),
            P(None, "tp"),
            P("tp", "fs"),
        ),
        out_specs=P(("rep", "fs"), "tp"),
        check_vma=False,
    )
```

```python
import jax
import jax.numpy as jnp
from jax import lax
from jax.experimental import pallas as pl
from jax.experimental.pallas import tpu as pltpu
from jax.sharding import PartitionSpec as P

TAPS = 3
EPSILON = 1e-06
Z_LO, Z_ALL, Y = 8, 16, 4
ROWS = 64
PARTS = (
    ((0, 640, "y"), (640, 768, "z")),
    ((0, 256, "y"), (256, 512, "z")),
    ((0, 128, "y"), (128, 384, "z")),
)
WIDTHS = (1408, 768, 512)
RATE = 46.6e3
HOP = 2.0
AHEAD = 4.0
X_COPIES = 9 * 3 + 10 * 3 + 8


class Copy:
    def __init__(self, number, part, link, dz, dy, row, rows, after):
        self.number, self.part, self.link = number, part, link
        self.dz, self.dy, self.row, self.rows = dz, dy, row, rows
        self.after, self.tail = after, 0.0
        stream, index = part
        self.time = rows * PARTS[stream][index][1] * 2 / RATE
        self.start = None


def all_copies():
    copies = []

    def add(part, link, dz, dy, after, row=0, rows=ROWS):
        copies.append(Copy(len(copies), part, link, dz, dy, row, rows, list(after)))
        return copies[-1]

    half = ROWS // 2
    for stream, parts in enumerate(PARTS):
        for index, (_, _, first) in enumerate(parts):
            part = (stream, index)

            def along_z(dy, own):
                came = {0: own}
                for sign, link, row in ((-1, "z+", 0), (1, "z-", half)):
                    previous = own
                    for step in range(3):
                        previous = [add(part, link, sign * step, dy, previous)]
                        came[sign * (step + 1)] = previous
                    last = add(part, link, sign * 3, dy, previous, row, half)
                    came.setdefault(4, []).append(last)
                return came

            def along_y(dz, own):
                up = add(part, "y+", dz, 0, own)
                down = add(part, "y-", dz, 0, own)
                far = [
                    add(part, "y+", dz, -1, [up], 0, half),
                    add(part, "y-", dz, 1, [down], half, half),
                ]
                return {0: own, -1: [up], 1: [down], 2: far}

            if first == "y":
                for dy, got in along_y(0, []).items():
                    along_z(dy, got)
            else:
                for dz, got in along_z(0, []).items():
                    along_y(dz, got)
    for copy in reversed(copies):
        for before in copy.after:
            before.tail = max(before.tail, copy.tail + copy.time + HOP)
    return copies


def planned():
    copies = all_copies()
    free = dict.fromkeys(("y+", "y-", "z+", "z-"), 0.0)
    waiting, flying, here, order, now = list(copies), [], set(), [], 0.0
    while waiting or flying:
        ready = [c for c in waiting if all(b.number in here for b in c.after)]
        ready.sort(key=lambda c: (c.part[0], -c.tail, c.number))
        for copy in ready:
            if free[copy.link] < now + AHEAD:
                free[copy.link] = max(free[copy.link], now) + copy.time
                flying.append((free[copy.link] + HOP, copy.number, copy))
                waiting.remove(copy)
                order.append(("start", copy, now))
        flying.sort(key=lambda f: f[:2])
        now, _, copy = flying.pop(0)
        here.add(copy.number)
        order.append(("wait", copy, now))
    return order, copies


MESH = pl.DeviceIdType.MESH
TOK, D, SLOTS, SLICE = 256, 2048, 8, 256
UNITS, CHANNELS = 704, 128
F32, BF16 = jnp.float32, jnp.bfloat16


def turned_dot(x, turned):
    return lax.dot_general(x, turned, (((1,), (1,)), ((), ())), preferred_element_type=F32)


def layer_kernel(order, copies, refs):
    (stream, gains, own0, own1, own2, taps, out, full0, full1, full2, send_sem, recv_sem, x_send,
     x_recv, act, first, second, branch1, branch2, normed, hidden, acc, pair_out, pair_in, far_out,
     far_in, near_out, near_in, conv, halo_out, halo_in, sq_out, sq_in) = refs
    own, full = (own0, own1, own2), (full0, full1, full2)
    rep, fs, tp = lax.axis_index("rep"), lax.axis_index("fs"), lax.axis_index("tp")
    z_lo, y = fs // Y, lax.rem(fs, Y)
    z = rep * Z_LO + z_lo
    x, core = tp // 2, lax.rem(tp, 2)

    def at(z_to, y_to):
        return (z_to // Z_LO, lax.rem(z_to, Z_LO) * Y + y_to, tp)

    def peer(slot):
        return (rep, fs, slot)

    def slot_of(dx, dc=0):
        return lax.rem(x + dx, 4) * 2 + (core if dc == 0 else 1 - core)

    place = {
        "y+": at(z, lax.rem(y + 1, Y)),
        "y-": at(z, lax.rem(y + Y - 1, Y)),
        "z+": at(lax.rem(z + 1, Z_ALL), y),
        "z-": at(lax.rem(z + Z_ALL - 1, Z_ALL), y),
    }
    up, down, partner = peer(slot_of(1)), peer(slot_of(3)), peer(slot_of(0, 1))
    after = (z * Y + y + 1 + Z_ALL * Y) % (Z_ALL * Y)
    before = (z * Y + y - 1 + Z_ALL * Y) % (Z_ALL * Y)
    next_place = at(after // Y, lax.rem(after, Y))
    last_place = at(before // Y, lax.rem(before, Y))
    others = [peer(lax.rem(tp + i, SLOTS)) for i in range(1, SLOTS)]

    barrier = pltpu.get_barrier_semaphore()
    greeted = [*place.values(), *others, next_place, last_place]
    for device in greeted:
        pl.semaphore_signal(barrier, inc=1, device_id=device, device_id_type=MESH)
    pl.semaphore_wait(barrier, len(greeted))

    def remote(copy):
        stream_, index = copy.part
        column, width, _ = PARTS[stream_][index]
        columns = pl.ds(column, width)
        block = lax.rem(z_lo + copy.dz + Z_LO, Z_LO) * Y + lax.rem(y + copy.dy + Y, Y)
        rows = pl.ds(pl.multiple_of(block * ROWS, ROWS) + copy.row, copy.rows)
        target = full[stream_].at[rows, columns]
        source = target
        if copy.dz == 0 and copy.dy == 0:
            source = own[stream_].at[pl.ds(copy.row, copy.rows), columns]
        return pltpu.make_async_remote_copy(
            src_ref=source,
            dst_ref=target,
            send_sem=send_sem.at[copy.number],
            recv_sem=recv_sem.at[copy.number],
            device_id=place[copy.link],
            device_id_type=MESH,
        )

    events = list(order)

    def pump(until):
        while events and events[0][2] <= until:
            kind, copy, _ = events.pop(0)
            if kind == "start":
                remote(copy).start()
            else:
                remote(copy).wait_recv()

    sent = []

    def send(source, target, device):
        number = len(sent)
        copy = pltpu.make_async_remote_copy(
            src_ref=source,
            dst_ref=target,
            send_sem=x_send.at[number],
            recv_sem=x_recv.at[number],
            device_id=device,
            device_id_type=MESH,
        )
        copy.start()
        sent.append(copy)
        return copy

    def gather_x(buffer, source, pace=lambda step: None):
        half = TOK // 2
        low, high = pl.ds(0, half), pl.ds(half, half)
        mine, left, right, far = slot_of(0), slot_of(3), slot_of(1), slot_of(2)

        def same(ref, device):
            return send(ref, ref, device)

        from_left = send(source, buffer.at[mine], up)
        from_right = send(source, buffer.at[mine], down)
        pairs = [send(source, buffer.at[mine], partner)]
        pace(0)
        from_left.wait_recv()
        far_low = same(buffer.at[left, low], up)
        pairs.append(same(buffer.at[left], partner))
        from_right.wait_recv()
        far_high = same(buffer.at[right, high], down)
        pairs.append(same(buffer.at[right], partner))
        pace(1)
        far_low.wait_recv()
        pairs.append(same(buffer.at[far, low], partner))
        far_high.wait_recv()
        pairs.append(same(buffer.at[far, high], partner))
        pace(2)
        for copy in pairs:
            copy.wait_recv()

    def reduce_x(use, product):
        half = TOK // 2
        low, high = pl.ds(0, half), pl.ds(half, half)
        pair = {}
        for d in (2, 1, 3, 0):
            pair_out[use, d] = product(slot_of(d, 1)).astype(BF16)
            pair[d] = send(pair_out.at[use, d], pair_in.at[use, d], partner)
        for d in (2, 1, 3, 0):
            acc[d] = product(slot_of(d))

        def chip_sum(d, rows):
            return acc[d, rows] + pair_in[use, d, rows].astype(F32)

        pair[2].wait_recv()
        far_out[use, 0] = chip_sum(2, low).astype(BF16)
        far_low = send(far_out.at[use, 0], far_in.at[use, 0], up)
        far_out[use, 1] = chip_sum(2, high).astype(BF16)
        far_high = send(far_out.at[use, 1], far_in.at[use, 1], down)
        pair[1].wait_recv()
        near_out[use, 0, high] = chip_sum(1, high).astype(BF16)
        near = [send(near_out.at[use, 0, high], near_in.at[use, 0, high], up)]
        pair[3].wait_recv()
        near_out[use, 1, low] = chip_sum(3, low).astype(BF16)
        near.append(send(near_out.at[use, 1, low], near_in.at[use, 1, low], down))
        pair[0].wait_recv()
        far_low.wait_recv()
        near_out[use, 0, low] = (chip_sum(1, low) + far_in[use, 0].astype(F32)).astype(BF16)
        near.append(send(near_out.at[use, 0, low], near_in.at[use, 0, low], up))
        far_high.wait_recv()
        near_out[use, 1, high] = (chip_sum(3, high) + far_in[use, 1].astype(F32)).astype(BF16)
        near.append(send(near_out.at[use, 1, high], near_in.at[use, 1, high], down))
        for copy in near:
            copy.wait_recv()
        total = acc[0] + pair_in[use, 0].astype(F32)
        return total + near_in[use, 0].astype(F32) + near_in[use, 1].astype(F32)

    def scale_of(squares):
        return lax.rsqrt(squares / D + EPSILON)

    def squares_of(values):
        return jnp.sum(values * values, axis=1, keepdims=True)

    def normalize(buffer, row):
        squares = jnp.zeros((TOK, 1), F32)
        for j in range(SLOTS):
            squares = squares + squares_of(buffer[j].astype(F32))
        scale = scale_of(squares)
        for j in range(SLOTS):
            values = buffer[j].astype(F32) * scale * gains[row, j]
            normed[:, j * SLICE : (j + 1) * SLICE] = values.astype(BF16)

    def settle(current, branch, row, weight, result):
        squares = jnp.zeros((TOK, 1), F32)
        for j in range(SLOTS):
            squares = squares + squares_of(branch[j].astype(F32))
        scale = scale_of(squares)
        for j in range(SLOTS):
            step = branch[j].astype(F32) * scale * gains[row, j]
            result[j] = (current[j].astype(F32) + weight * step).astype(BF16)

    def silu(v):
        return v / (1.0 + jnp.exp(-v))

    def gate_and_up():
        def block(i, _):
            columns = pl.ds(pl.multiple_of(i * 256, 256), 256)
            both = jnp.dot(normed[...], full0[:, columns], preferred_element_type=F32)
            value = silu(both[:, :128]) * both[:, 128:]
            hidden[:, pl.ds(pl.multiple_of(i * 128, 128), 128)] = value.astype(BF16)
            return 0

        lax.fori_loop(0, 5, block, 0)
        both = jnp.dot(normed[...], full0[:, 1280:1408], preferred_element_type=F32)
        value = silu(both) * pltpu.roll(both, 64, 1)
        lane = lax.broadcasted_iota(jnp.int32, value.shape, 1)
        hidden[:, 640:768] = jnp.where(lane < 64, value, 0.0).astype(BF16)

    def slot_rows(slot):
        return pl.ds(pl.multiple_of(slot * SLICE, SLICE), SLICE)

    def down_product(slot):
        return turned_dot(hidden[...], full1[slot_rows(slot), :])

    act[tp] = stream[...]
    mine = pl.ds(pl.multiple_of(fs * ROWS, ROWS), ROWS)
    pump(0.0)
    for s in range(3):
        full[s][mine, :] = own[s][...]
    gather_x(act, stream, lambda step: pump((3.0, 6.0, 9.0)[step]))
    normalize(act, 0)
    both_here = max(t for kind, c, t in order if kind == "wait" and c.part[0] == 0)
    pump(both_here)
    gate_and_up()
    pump(1e9)

    branch1[tp] = reduce_x(0, down_product).astype(BF16)
    gather_x(branch1, branch1.at[tp])
    settle(act, branch1, 1, 0.5, first)

    normalize(first, 2)
    mix_in = jnp.dot(normed[...], full2[:, : 3 * CHANNELS], preferred_element_type=F32)
    conv_input = mix_in[:, 2 * CHANNELS :] * mix_in[:, :CHANNELS]
    conv[8:] = conv_input
    halo_out[...] = conv_input[TOK - 8 :]
    halo = send(halo_out, halo_in, next_place)
    halo.wait_recv()
    conv[:8] = jnp.where(fs == 0, 0.0, halo_in[...])
    mixed = taps[0:1, :] * conv[6 : 6 + TOK]
    for tap in range(1, TAPS):
        mixed = mixed + taps[tap : tap + 1, :] * conv[6 + tap : 6 + tap + TOK]
    hidden[:, :CHANNELS] = (mix_in[:, CHANNELS : 2 * CHANNELS] * mixed).astype(BF16)

    def out_product(slot):
        return turned_dot(hidden[:, :CHANNELS], full2[slot_rows(slot), 3 * CHANNELS :])

    branch2[tp] = reduce_x(1, out_product).astype(BF16)
    gather_x(branch2, branch2.at[tp])
    settle(first, branch2, 3, 1.0, second)

    normalize(second, 4)
    gate_and_up()
    branch = reduce_x(2, down_product)
    squares = jnp.broadcast_to(squares_of(branch), (TOK, 128))
    sq_out[...] = jnp.transpose(squares)[:8]
    got = [send(sq_out, sq_in.at[i], device) for i, device in enumerate(others)]
    total = sq_out[...]
    for copy in got:
        copy.wait_recv()
    for i in range(SLOTS - 1):
        total = total + sq_in[i]
    scale = jnp.transpose(scale_of(jnp.concatenate([total] * 16, axis=0)))[:, :1]
    step = branch * scale * gains[5, tp]
    out[...] = (second[tp].astype(F32) + 0.5 * step).astype(BF16)

    for copy in copies:
        remote(copy).wait_send()
    for copy in sent:
        copy.wait_send()


def whole_layer(stream, gains, pieces, taps):
    order, copies = planned()

    def kernel(*refs):
        layer_kernel(order, copies, refs)

    slots = (SLOTS, TOK, SLICE)
    half = TOK // 2
    scratch = [pltpu.VMEM((ROWS * Z_LO * Y, w), BF16) for w in WIDTHS]
    scratch += [pltpu.SemaphoreType.DMA((len(copies),))] * 2
    scratch += [pltpu.SemaphoreType.DMA((X_COPIES,))] * 2
    scratch += [pltpu.VMEM(slots, BF16)] * 5
    scratch += [
        pltpu.VMEM((TOK, D), BF16),
        pltpu.VMEM((TOK, 768), BF16),
        pltpu.VMEM((4, TOK, SLICE), F32),
        pltpu.VMEM((3, 4, TOK, SLICE), BF16),
        pltpu.VMEM((3, 4, TOK, SLICE), BF16),
        pltpu.VMEM((3, 2, half, SLICE), BF16),
        pltpu.VMEM((3, 2, half, SLICE), BF16),
        pltpu.VMEM((3, 2, TOK, SLICE), BF16),
        pltpu.VMEM((3, 2, TOK, SLICE), BF16),
        pltpu.VMEM((TOK + 8, CHANNELS), F32),
        pltpu.VMEM((8, CHANNELS), F32),
        pltpu.VMEM((8, CHANNELS), F32),
        pltpu.VMEM((8, TOK), F32),
        pltpu.VMEM((SLOTS - 1, 8, TOK), F32),
    ]
    return pl.pallas_call(
        kernel,
        out_shape=jax.ShapeDtypeStruct(stream.shape, BF16),
        in_specs=[pl.BlockSpec(memory_space=pltpu.VMEM)] * 6,
        out_specs=pl.BlockSpec(memory_space=pltpu.VMEM),
        scratch_shapes=scratch,
        compiler_params=pltpu.CompilerParams(
            collective_id=0, has_side_effects=True, vmem_limit_bytes=60 * 2**20
        ),
    )(stream, gains, *pieces, taps)


def packed(w_gate, w_up, w_down, w_inner, w_bgate, w_cgate, w_out):
    blocks = []
    for at in range(0, UNITS, 128):
        blocks += [w_gate[:, at : at + 128], w_up[:, at : at + 128]]
    first = jnp.concatenate(blocks, axis=1)
    second = jnp.pad(w_down.T, ((0, 0), (0, 64)))
    third = jnp.concatenate([w_inner, w_bgate, w_cgate, w_out.T], axis=1)
    return first, second, third


def shards(stream, norm_gains, w_gate, w_up, w_down, w_inner, w_bgate, w_cgate, conv_taps, w_out):
    pieces = packed(w_gate, w_up, w_down, w_inner, w_bgate, w_cgate, w_out)
    gains = norm_gains.reshape(-1, SLOTS, 1, SLICE)
    return whole_layer(stream, gains, pieces, conv_taps)


def solution(mesh):
    return jax.shard_map(
        shards,
        mesh=mesh,
        in_specs=(
            P(("rep", "fs"), "tp"),
            P(),
            P("fs", "tp"),
            P("fs", "tp"),
            P("tp", "fs"),
            P("fs", "tp"),
            P("fs", "tp"),
            P("fs", "tp"),
            P(None, "tp"),
            P("tp", "fs"),
        ),
        out_specs=P(("rep", "fs"), "tp"),
        check_vma=False,
    )
```

```python
import jax
import jax.numpy as jnp
from jax import lax
from jax.experimental import pallas as pl
from jax.experimental.pallas import tpu as pltpu
from jax.sharding import PartitionSpec as P

TAPS = 3
EPSILON = 1e-06
Z_LO, Z_ALL, Y = 8, 16, 4
ROWS = 64
PARTS = (
    ((0, 896, "y"), (896, 1280, "z")),
    ((0, 128, "y"), (128, 384, "z")),
)
WIDTHS = (2176, 512)
RATE = 52e3
HOP = 2.8
AHEAD = 6.0
X_COPIES = 9 * 3 + 10 * 3 + 8


class Copy:
    def __init__(self, number, part, link, dz, dy, row, rows, after):
        self.number, self.part, self.link = number, part, link
        self.dz, self.dy, self.row, self.rows = dz, dy, row, rows
        self.after, self.tail = after, 0.0
        stream, index = part
        self.time = rows * PARTS[stream][index][1] * 2 / RATE
        self.start = None


def all_copies():
    copies = []

    def add(part, link, dz, dy, after, row=0, rows=ROWS):
        copies.append(Copy(len(copies), part, link, dz, dy, row, rows, list(after)))
        return copies[-1]

    half = ROWS // 2
    for stream, parts in enumerate(PARTS):
        for index, (_, _, first) in enumerate(parts):
            part = (stream, index)

            def along_z(dy, own):
                came = {0: own}
                for sign, link, row in ((-1, "z+", 0), (1, "z-", half)):
                    previous = own
                    for step in range(3):
                        previous = [add(part, link, sign * step, dy, previous)]
                        came[sign * (step + 1)] = previous
                    last = add(part, link, sign * 3, dy, previous, row, half)
                    came.setdefault(4, []).append(last)
                return came

            def along_y(dz, own):
                up = add(part, "y+", dz, 0, own)
                down = add(part, "y-", dz, 0, own)
                far = [
                    add(part, "y+", dz, -1, [up], 0, half),
                    add(part, "y-", dz, 1, [down], half, half),
                ]
                return {0: own, -1: [up], 1: [down], 2: far}

            if first == "y":
                for dy, got in along_y(0, []).items():
                    along_z(dy, got)
            else:
                for dz, got in along_z(0, []).items():
                    along_y(dz, got)
    for copy in reversed(copies):
        for before in copy.after:
            before.tail = max(before.tail, copy.tail + copy.time + HOP)
    return copies


def planned():
    copies = all_copies()
    free = dict.fromkeys(("y+", "y-", "z+", "z-"), 0.0)
    waiting, flying, here, order, now = list(copies), [], set(), [], 0.0
    while waiting or flying:
        ready = [c for c in waiting if all(b.number in here for b in c.after)]
        ready.sort(key=lambda c: (c.part[0], -c.tail, c.number))
        for copy in ready:
            if free[copy.link] < now + AHEAD:
                free[copy.link] = max(free[copy.link], now) + copy.time
                flying.append((free[copy.link] + HOP, copy.number, copy))
                waiting.remove(copy)
                order.append(("start", copy, now))
        flying.sort(key=lambda f: f[:2])
        now, _, copy = flying.pop(0)
        here.add(copy.number)
        order.append(("wait", copy, now))
    return order, copies


MESH = pl.DeviceIdType.MESH
TOK, D, SLOTS, SLICE = 256, 2048, 8, 256
UNITS, CHANNELS = 704, 128
F32, BF16 = jnp.float32, jnp.bfloat16


def turned_dot(x, turned):
    return lax.dot_general(x, turned, (((1,), (1,)), ((), ())), preferred_element_type=F32)


def layer_kernel(order, copies, refs):
    (stream, gains, w_gate, w_up, w_down, w_inner, w_bgate, w_cgate, w_out, taps, out, full0, full1,
     send_sem, recv_sem, x_send, x_recv, act, first, second, branch1, branch2, normed, hidden, acc,
     pair_out, pair_in, far_out, far_in, near_out, near_in, conv, halo_out, halo_in, sq_out,
     sq_in) = refs
    full = (full0, full1)
    rep, fs, tp = lax.axis_index("rep"), lax.axis_index("fs"), lax.axis_index("tp")
    z_lo, y = fs // Y, lax.rem(fs, Y)
    z = rep * Z_LO + z_lo
    x, core = tp // 2, lax.rem(tp, 2)

    def at(z_to, y_to):
        return (z_to // Z_LO, lax.rem(z_to, Z_LO) * Y + y_to, tp)

    def peer(slot):
        return (rep, fs, slot)

    def slot_of(dx, dc=0):
        return lax.rem(x + dx, 4) * 2 + (core if dc == 0 else 1 - core)

    place = {
        "y+": at(z, lax.rem(y + 1, Y)),
        "y-": at(z, lax.rem(y + Y - 1, Y)),
        "z+": at(lax.rem(z + 1, Z_ALL), y),
        "z-": at(lax.rem(z + Z_ALL - 1, Z_ALL), y),
    }
    up, down, partner = peer(slot_of(1)), peer(slot_of(3)), peer(slot_of(0, 1))
    after = (z * Y + y + 1 + Z_ALL * Y) % (Z_ALL * Y)
    before = (z * Y + y - 1 + Z_ALL * Y) % (Z_ALL * Y)
    next_place = at(after // Y, lax.rem(after, Y))
    last_place = at(before // Y, lax.rem(before, Y))
    others = [peer(lax.rem(tp + i, SLOTS)) for i in range(1, SLOTS)]

    mine = pl.ds(pl.multiple_of(fs * ROWS, ROWS), ROWS)
    for i in range(5):
        columns = slice(128 * i, 128 * i + 128)
        full0[mine, 256 * i : 256 * i + 128] = w_gate[:, columns]
        full0[mine, 256 * i + 128 : 256 * i + 256] = w_up[:, columns]
    full0[mine, 1280:1408] = jnp.concatenate([w_gate[:, 640:], w_up[:, 640:]], axis=1)
    full0[mine, 1408:2048] = w_down[:, :640]
    rest = jnp.concatenate([w_down[:, 640:], jnp.zeros((ROWS, 64), BF16)], axis=1)
    full0[mine, 2048:2176] = rest
    full1[mine, :128] = w_inner[...]
    full1[mine, 128:256] = w_bgate[...]
    full1[mine, 256:384] = w_cgate[...]
    full1[mine, 384:] = w_out[...]
    act[tp] = stream[...]

    barrier = pltpu.get_barrier_semaphore()
    greeted = [*place.values(), *others, next_place, last_place]
    for device in greeted:
        pl.semaphore_signal(barrier, inc=1, device_id=device, device_id_type=MESH)
    pl.semaphore_wait(barrier, len(greeted))

    def remote(copy):
        stream_, index = copy.part
        column, width, _ = PARTS[stream_][index]
        columns = pl.ds(column, width)
        block = lax.rem(z_lo + copy.dz + Z_LO, Z_LO) * Y + lax.rem(y + copy.dy + Y, Y)
        rows = pl.ds(pl.multiple_of(block * ROWS, ROWS) + copy.row, copy.rows)
        target = full[stream_].at[rows, columns]
        return pltpu.make_async_remote_copy(
            src_ref=target,
            dst_ref=target,
            send_sem=send_sem.at[copy.number],
            recv_sem=recv_sem.at[copy.number],
            device_id=place[copy.link],
            device_id_type=MESH,
        )

    events = list(order)

    def pump(until):
        while events and events[0][2] <= until:
            kind, copy, _ = events.pop(0)
            if kind == "start":
                remote(copy).start()
            else:
                remote(copy).wait_recv()

    sent = []

    def send(source, target, device):
        number = len(sent)
        copy = pltpu.make_async_remote_copy(
            src_ref=source,
            dst_ref=target,
            send_sem=x_send.at[number],
            recv_sem=x_recv.at[number],
            device_id=device,
            device_id_type=MESH,
        )
        copy.start()
        sent.append(copy)
        return copy

    def gather_x(buffer, source, pace=lambda step: None):
        half = TOK // 2
        low, high = pl.ds(0, half), pl.ds(half, half)
        mine, left, right, far = slot_of(0), slot_of(3), slot_of(1), slot_of(2)

        def same(ref, device):
            return send(ref, ref, device)

        from_left = send(source, buffer.at[mine], up)
        from_right = send(source, buffer.at[mine], down)
        pairs = [send(source, buffer.at[mine], partner)]
        pace(0)
        from_left.wait_recv()
        far_low = same(buffer.at[left, low], up)
        pairs.append(same(buffer.at[left], partner))
        from_right.wait_recv()
        far_high = same(buffer.at[right, high], down)
        pairs.append(same(buffer.at[right], partner))
        pace(1)
        far_low.wait_recv()
        pairs.append(same(buffer.at[far, low], partner))
        far_high.wait_recv()
        pairs.append(same(buffer.at[far, high], partner))
        pace(2)
        for copy in pairs:
            copy.wait_recv()

    def reduce_x(use, product, pace=lambda step: None):
        half = TOK // 2
        low, high = pl.ds(0, half), pl.ds(half, half)
        pair = {}
        for d in (2, 1, 3, 0):
            pair_out[use, d] = product(slot_of(d, 1)).astype(BF16)
            pair[d] = send(pair_out.at[use, d], pair_in.at[use, d], partner)
        pace(0)
        for d in (2, 1, 3, 0):
            acc[d] = product(slot_of(d))
        pace(1)

        def chip_sum(d, rows):
            return acc[d, rows] + pair_in[use, d, rows].astype(F32)

        pair[2].wait_recv()
        far_out[use, 0] = chip_sum(2, low).astype(BF16)
        far_low = send(far_out.at[use, 0], far_in.at[use, 0], up)
        far_out[use, 1] = chip_sum(2, high).astype(BF16)
        far_high = send(far_out.at[use, 1], far_in.at[use, 1], down)
        pace(2)
        pair[1].wait_recv()
        near_out[use, 0, high] = chip_sum(1, high).astype(BF16)
        near = [send(near_out.at[use, 0, high], near_in.at[use, 0, high], up)]
        pair[3].wait_recv()
        near_out[use, 1, low] = chip_sum(3, low).astype(BF16)
        near.append(send(near_out.at[use, 1, low], near_in.at[use, 1, low], down))
        pair[0].wait_recv()
        pace(3)
        far_low.wait_recv()
        near_out[use, 0, low] = (chip_sum(1, low) + far_in[use, 0].astype(F32)).astype(BF16)
        near.append(send(near_out.at[use, 0, low], near_in.at[use, 0, low], up))
        far_high.wait_recv()
        near_out[use, 1, high] = (chip_sum(3, high) + far_in[use, 1].astype(F32)).astype(BF16)
        near.append(send(near_out.at[use, 1, high], near_in.at[use, 1, high], down))
        pace(4)
        for copy in near:
            copy.wait_recv()
        total = acc[0] + pair_in[use, 0].astype(F32)
        return total + near_in[use, 0].astype(F32) + near_in[use, 1].astype(F32)

    def scale_of(squares):
        return lax.rsqrt(squares / D + EPSILON)

    def squares_of(values):
        return jnp.sum(values * values, axis=1, keepdims=True)

    def normalize(buffer, row):
        squares = jnp.zeros((TOK, 1), F32)
        for j in range(SLOTS):
            squares = squares + squares_of(buffer[j].astype(F32))
        scale = scale_of(squares)
        for j in range(SLOTS):
            values = buffer[j].astype(F32) * scale * gains[row : row + 1, j * SLICE : (j + 1) * SLICE]
            normed[:, j * SLICE : (j + 1) * SLICE] = values.astype(BF16)

    def settle(current, branch, row, weight, result):
        squares = jnp.zeros((TOK, 1), F32)
        for j in range(SLOTS):
            squares = squares + squares_of(branch[j].astype(F32))
        scale = scale_of(squares)
        for j in range(SLOTS):
            step = branch[j].astype(F32) * scale * gains[row : row + 1, j * SLICE : (j + 1) * SLICE]
            result[j] = (current[j].astype(F32) + weight * step).astype(BF16)

    def silu(v):
        return v / (1.0 + jnp.exp(-v))

    def gate_and_up():
        def block(i, _):
            columns = pl.ds(pl.multiple_of(i * 256, 256), 256)
            both = jnp.dot(normed[...], full0[:, columns], preferred_element_type=F32)
            value = silu(both[:, :128]) * both[:, 128:]
            hidden[:, pl.ds(pl.multiple_of(i * 128, 128), 128)] = value.astype(BF16)
            return 0

        lax.fori_loop(0, 5, block, 0)
        both = jnp.dot(normed[...], full0[:, 1280:1408], preferred_element_type=F32)
        value = silu(both) * pltpu.roll(both, 64, 1)
        lane = lax.broadcasted_iota(jnp.int32, value.shape, 1)
        hidden[:, 640:768] = jnp.where(lane < 64, value, 0.0).astype(BF16)

    def slot_rows(slot):
        return pl.ds(pl.multiple_of(slot * SLICE, SLICE), SLICE)

    def down_product(slot):
        return turned_dot(hidden[...], full0[slot_rows(slot), 1408:])

    pump(0.0)
    gather_x(act, stream, lambda step: pump((3.0, 6.0, 9.0)[step]))
    normalize(act, 0)
    here = max(t for kind, c, t in order if kind == "wait" and c.part[0] == 0)
    pump(here)
    gate_and_up()
    pump(here + 2.5)
    branch1[tp] = reduce_x(
        0, down_product, lambda step: pump(here + (3.3, 4.2, 5.0, 6.0, 9.5)[step])
    ).astype(BF16)
    gather_x(branch1, branch1.at[tp], lambda step: pump(here + (12.0, 16.0, 1e9)[step]))
    settle(act, branch1, 1, 0.5, first)

    normalize(first, 2)
    mix_in = jnp.dot(normed[...], full1[:, : 3 * CHANNELS], preferred_element_type=F32)
    conv_input = mix_in[:, 2 * CHANNELS :] * mix_in[:, :CHANNELS]
    conv[8:] = conv_input
    halo_out[...] = conv_input[TOK - 8 :]
    halo = send(halo_out, halo_in, next_place)
    halo.wait_recv()
    conv[:8] = jnp.where(fs == 0, 0.0, halo_in[...])
    mixed = taps[0:1, :] * conv[6 : 6 + TOK]
    for tap in range(1, TAPS):
        mixed = mixed + taps[tap : tap + 1, :] * conv[6 + tap : 6 + tap + TOK]
    hidden[:, :CHANNELS] = (mix_in[:, CHANNELS : 2 * CHANNELS] * mixed).astype(BF16)

    def out_product(slot):
        return turned_dot(hidden[:, :CHANNELS], full1[slot_rows(slot), 3 * CHANNELS :])

    branch2[tp] = reduce_x(1, out_product).astype(BF16)
    gather_x(branch2, branch2.at[tp])
    settle(first, branch2, 3, 1.0, second)

    normalize(second, 4)
    gate_and_up()
    branch = reduce_x(2, down_product)
    squares = jnp.broadcast_to(squares_of(branch), (TOK, 128))
    sq_out[...] = jnp.transpose(squares)[:8]
    got = [send(sq_out, sq_in.at[i], device) for i, device in enumerate(others)]
    total = sq_out[...]
    for copy in got:
        copy.wait_recv()
    for i in range(SLOTS - 1):
        total = total + sq_in[i]
    scale = jnp.transpose(scale_of(jnp.concatenate([total] * 16, axis=0)))[:, :1]
    step = branch * scale * gains[5:6, pl.ds(pl.multiple_of(tp * SLICE, SLICE), SLICE)]
    out[...] = (second[tp].astype(F32) + 0.5 * step).astype(BF16)

    for copy in copies:
        remote(copy).wait_send()
    for copy in sent:
        copy.wait_send()


def whole_layer(*arrays):
    order, copies = planned()

    def kernel(*refs):
        layer_kernel(order, copies, refs)

    slots = (SLOTS, TOK, SLICE)
    half = TOK // 2
    scratch = [pltpu.VMEM((ROWS * Z_LO * Y, w), BF16) for w in WIDTHS]
    scratch += [pltpu.SemaphoreType.DMA((len(copies),))] * 2
    scratch += [pltpu.SemaphoreType.DMA((X_COPIES,))] * 2
    scratch += [pltpu.VMEM(slots, BF16)] * 5
    scratch += [
        pltpu.VMEM((TOK, D), BF16),
        pltpu.VMEM((TOK, 768), BF16),
        pltpu.VMEM((4, TOK, SLICE), F32),
        pltpu.VMEM((3, 4, TOK, SLICE), BF16),
        pltpu.VMEM((3, 4, TOK, SLICE), BF16),
        pltpu.VMEM((3, 2, half, SLICE), BF16),
        pltpu.VMEM((3, 2, half, SLICE), BF16),
        pltpu.VMEM((3, 2, TOK, SLICE), BF16),
        pltpu.VMEM((3, 2, TOK, SLICE), BF16),
        pltpu.VMEM((TOK + 8, CHANNELS), F32),
        pltpu.VMEM((8, CHANNELS), F32),
        pltpu.VMEM((8, CHANNELS), F32),
        pltpu.VMEM((8, TOK), F32),
        pltpu.VMEM((SLOTS - 1, 8, TOK), F32),
    ]
    return pl.pallas_call(
        kernel,
        out_shape=jax.ShapeDtypeStruct(arrays[0].shape, BF16),
        in_specs=[pl.BlockSpec(memory_space=pltpu.VMEM)] * len(arrays),
        out_specs=pl.BlockSpec(memory_space=pltpu.VMEM),
        scratch_shapes=scratch,
        compiler_params=pltpu.CompilerParams(
            collective_id=0, has_side_effects=True, vmem_limit_bytes=60 * 2**20
        ),
    )(*arrays)


def shards(stream, norm_gains, w_gate, w_up, w_down, w_inner, w_bgate, w_cgate, conv_taps, w_out):
    return whole_layer(
        stream, norm_gains, w_gate, w_up, w_down.T, w_inner, w_bgate, w_cgate, w_out.T, conv_taps
    )


def solution(mesh):
    return jax.shard_map(
        shards,
        mesh=mesh,
        in_specs=(
            P(("rep", "fs"), "tp"),
            P(),
            P("fs", "tp"),
            P("fs", "tp"),
            P("tp", "fs"),
            P("fs", "tp"),
            P("fs", "tp"),
            P("fs", "tp"),
            P(None, "tp"),
            P("tp", "fs"),
        ),
        out_specs=P(("rep", "fs"), "tp"),
        check_vma=False,
    )
```

```python
import jax
import jax.numpy as jnp
from jax import lax
from jax.experimental import pallas as pl
from jax.experimental.pallas import tpu as pltpu
from jax.sharding import PartitionSpec as P

TAPS = 3
EPSILON = 1e-06
Z_LO, Z_ALL, Y = 8, 16, 4
ROWS = 64
PARTS = (
    ((0, 896, "y"), (896, 1280, "z")),
    ((0, 128, "y"), (128, 384, "z")),
)
WIDTHS = (2176, 512)
RATE = 52e3
HOP = 2.8
AHEAD = (2.5, 2.5)
LATER = 8
X_COPIES = 13 * 3 + 10 * 3 + 8


class Copy:
    def __init__(self, number, part, link, dz, dy, row, rows, after):
        self.number, self.part, self.link = number, part, link
        self.dz, self.dy, self.row, self.rows = dz, dy, row, rows
        self.after, self.tail = after, 0.0
        stream, index = part
        self.time = rows * PARTS[stream][index][1] * 2 / RATE
        self.start = None


def all_copies():
    copies = []

    def add(part, link, dz, dy, after, row=0, rows=ROWS):
        copies.append(Copy(len(copies), part, link, dz, dy, row, rows, list(after)))
        return copies[-1]

    half = ROWS // 2
    for stream, parts in enumerate(PARTS):
        for index, (_, _, first) in enumerate(parts):
            part = (stream, index)

            def along_z(dy, own):
                came = {0: own}
                for sign, link, row in ((-1, "z+", 0), (1, "z-", half)):
                    previous = own
                    for step in range(3):
                        previous = [add(part, link, sign * step, dy, previous)]
                        came[sign * (step + 1)] = previous
                    last = add(part, link, sign * 3, dy, previous, row, half)
                    came.setdefault(4, []).append(last)
                return came

            def along_y(dz, own):
                up = add(part, "y+", dz, 0, own)
                down = add(part, "y-", dz, 0, own)
                far = [
                    add(part, "y+", dz, -1, [up], 0, half),
                    add(part, "y-", dz, 1, [down], half, half),
                ]
                return {0: own, -1: [up], 1: [down], 2: far}

            if first == "y":
                for dy, got in along_y(0, []).items():
                    along_z(dy, got)
            else:
                for dz, got in along_z(0, []).items():
                    along_y(dz, got)
    for copy in reversed(copies):
        for before in copy.after:
            before.tail = max(before.tail, copy.tail + copy.time + HOP)
    return copies


def planned():
    copies = all_copies()
    free = dict.fromkeys(("y+", "y-", "z+", "z-"), 0.0)
    waiting, flying, here, order, now = list(copies), [], set(), [], 0.0
    while waiting or flying:
        ready = [c for c in waiting if all(b.number in here for b in c.after)]
        ready.sort(key=lambda c: (c.part[0], -c.tail, c.number))
        for copy in ready:
            if copy.part[0] and sum(c.part[0] == 0 for c in waiting) > LATER:
                break
            if free[copy.link] < now + AHEAD[copy.part[0]]:
                free[copy.link] = max(free[copy.link], now) + copy.time
                flying.append((free[copy.link] + HOP, copy.number, copy))
                waiting.remove(copy)
                order.append(("start", copy, now))
        flying.sort(key=lambda f: f[:2])
        now, _, copy = flying.pop(0)
        here.add(copy.number)
        order.append(("wait", copy, now))
    return order, copies


MESH = pl.DeviceIdType.MESH
TOK, D, SLOTS, SLICE = 256, 2048, 8, 256
UNITS, CHANNELS = 704, 128
F32, BF16 = jnp.float32, jnp.bfloat16


def turned_dot(x, turned):
    return lax.dot_general(x, turned, (((1,), (1,)), ((), ())), preferred_element_type=F32)


def layer_kernel(order, copies, refs):
    (stream, gains, w_gate, w_up, w_down, w_inner, w_bgate, w_cgate, w_out, taps, out, full0, full1,
     send_sem, recv_sem, x_send, x_recv, act, first, second, branch1, branch2, normed, hidden, acc,
     pair_out, pair_in, far_out, far_in, near_out, near_in, conv, halo_out, halo_in, sq_out,
     sq_in) = refs
    full = (full0, full1)
    rep, fs, tp = lax.axis_index("rep"), lax.axis_index("fs"), lax.axis_index("tp")
    z_lo, y = fs // Y, lax.rem(fs, Y)
    z = rep * Z_LO + z_lo
    x, core = tp // 2, lax.rem(tp, 2)

    def at(z_to, y_to):
        return (z_to // Z_LO, lax.rem(z_to, Z_LO) * Y + y_to, tp)

    def peer(slot):
        return (rep, fs, slot)

    def slot_of(dx, dc=0):
        return lax.rem(x + dx, 4) * 2 + (core if dc == 0 else 1 - core)

    place = {
        "y+": at(z, lax.rem(y + 1, Y)),
        "y-": at(z, lax.rem(y + Y - 1, Y)),
        "z+": at(lax.rem(z + 1, Z_ALL), y),
        "z-": at(lax.rem(z + Z_ALL - 1, Z_ALL), y),
    }
    up, down, partner = peer(slot_of(1)), peer(slot_of(3)), peer(slot_of(0, 1))
    after = (z * Y + y + 1 + Z_ALL * Y) % (Z_ALL * Y)
    before = (z * Y + y - 1 + Z_ALL * Y) % (Z_ALL * Y)
    next_place = at(after // Y, lax.rem(after, Y))
    last_place = at(before // Y, lax.rem(before, Y))
    others = [peer(lax.rem(tp + i, SLOTS)) for i in range(1, SLOTS)]

    mine = pl.ds(pl.multiple_of(fs * ROWS, ROWS), ROWS)
    for i in range(5):
        columns = slice(128 * i, 128 * i + 128)
        full0[mine, 256 * i : 256 * i + 128] = w_gate[:, columns]
        full0[mine, 256 * i + 128 : 256 * i + 256] = w_up[:, columns]
    full0[mine, 1280:1408] = jnp.concatenate([w_gate[:, 640:], w_up[:, 640:]], axis=1)
    full0[mine, 1408:2048] = w_down[:, :640]
    rest = jnp.concatenate([w_down[:, 640:], jnp.zeros((ROWS, 64), BF16)], axis=1)
    full0[mine, 2048:2176] = rest
    full1[mine, :128] = w_inner[...]
    full1[mine, 128:256] = w_bgate[...]
    full1[mine, 256:384] = w_cgate[...]
    full1[mine, 384:] = w_out[...]
    act[tp] = stream[...]

    barrier = pltpu.get_barrier_semaphore()
    greeted = [*place.values(), *others, next_place, last_place]
    for device in greeted:
        pl.semaphore_signal(barrier, inc=1, device_id=device, device_id_type=MESH)
    pl.semaphore_wait(barrier, len(greeted))

    def remote(copy):
        stream_, index = copy.part
        column, width, _ = PARTS[stream_][index]
        columns = pl.ds(column, width)
        block = lax.rem(z_lo + copy.dz + Z_LO, Z_LO) * Y + lax.rem(y + copy.dy + Y, Y)
        rows = pl.ds(pl.multiple_of(block * ROWS, ROWS) + copy.row, copy.rows)
        target = full[stream_].at[rows, columns]
        return pltpu.make_async_remote_copy(
            src_ref=target,
            dst_ref=target,
            send_sem=send_sem.at[copy.number],
            recv_sem=recv_sem.at[copy.number],
            device_id=place[copy.link],
            device_id_type=MESH,
        )

    events = list(order)

    def pump(until):
        while events and events[0][2] <= until:
            kind, copy, _ = events.pop(0)
            if kind == "start":
                remote(copy).start()
            else:
                remote(copy).wait_recv()

    sent = []

    def send(source, target, device):
        number = len(sent)
        copy = pltpu.make_async_remote_copy(
            src_ref=source,
            dst_ref=target,
            send_sem=x_send.at[number],
            recv_sem=x_recv.at[number],
            device_id=device,
            device_id_type=MESH,
        )
        copy.start()
        sent.append(copy)
        return copy

    def gather_x(buffer, source, pace=lambda step: None):
        half = TOK // 2
        low, high = pl.ds(0, half), pl.ds(half, half)
        mine, left, right, far = slot_of(0), slot_of(3), slot_of(1), slot_of(2)

        def same(ref, device):
            return send(ref, ref, device)

        near = {}
        for rows_up, rows_down in ((low, high), (high, low)):
            for key, rows, device in (("left", rows_up, up), ("right", rows_down, down)):
                near.setdefault(key, []).append(
                    send(source.at[rows], buffer.at[mine, rows], device)
                )
        pairs = [send(source, buffer.at[mine], partner)]
        pace(0)
        near["left"][0].wait_recv()
        far_low = same(buffer.at[left, low], up)
        pairs.append(same(buffer.at[left, low], partner))
        near["right"][0].wait_recv()
        far_high = same(buffer.at[right, high], down)
        pairs.append(same(buffer.at[right, high], partner))
        near["left"][1].wait_recv()
        pairs.append(same(buffer.at[left, high], partner))
        near["right"][1].wait_recv()
        pairs.append(same(buffer.at[right, low], partner))
        pace(1)
        far_low.wait_recv()
        pairs.append(same(buffer.at[far, low], partner))
        far_high.wait_recv()
        pairs.append(same(buffer.at[far, high], partner))
        pace(2)
        for copy in pairs:
            copy.wait_recv()

    def reduce_x(use, product, pace=lambda step: None):
        half = TOK // 2
        low, high = pl.ds(0, half), pl.ds(half, half)
        pair = {}

        def give(d):
            pair_out[use, d] = product(slot_of(d, 1)).astype(BF16)
            pair[d] = send(pair_out.at[use, d], pair_in.at[use, d], partner)

        def chip_sum(d, rows):
            return acc[d, rows] + pair_in[use, d, rows].astype(F32)

        give(2)
        acc[2] = product(slot_of(2))
        give(1)
        give(3)
        give(0)
        pace(0)
        pair[2].wait_recv()
        far_out[use, 0] = chip_sum(2, low).astype(BF16)
        far_low = send(far_out.at[use, 0], far_in.at[use, 0], up)
        far_out[use, 1] = chip_sum(2, high).astype(BF16)
        far_high = send(far_out.at[use, 1], far_in.at[use, 1], down)
        pace(1)
        acc[1] = product(slot_of(1))
        pair[1].wait_recv()
        near_out[use, 0, high] = chip_sum(1, high).astype(BF16)
        near = [send(near_out.at[use, 0, high], near_in.at[use, 0, high], up)]
        acc[3] = product(slot_of(3))
        pair[3].wait_recv()
        near_out[use, 1, low] = chip_sum(3, low).astype(BF16)
        near.append(send(near_out.at[use, 1, low], near_in.at[use, 1, low], down))
        acc[0] = product(slot_of(0))
        pace(2)
        pair[0].wait_recv()
        pace(3)
        far_low.wait_recv()
        near_out[use, 0, low] = (chip_sum(1, low) + far_in[use, 0].astype(F32)).astype(BF16)
        near.append(send(near_out.at[use, 0, low], near_in.at[use, 0, low], up))
        far_high.wait_recv()
        near_out[use, 1, high] = (chip_sum(3, high) + far_in[use, 1].astype(F32)).astype(BF16)
        near.append(send(near_out.at[use, 1, high], near_in.at[use, 1, high], down))
        pace(4)
        for copy in near:
            copy.wait_recv()
        total = acc[0] + pair_in[use, 0].astype(F32)
        return total + near_in[use, 0].astype(F32) + near_in[use, 1].astype(F32)

    def scale_of(squares):
        return lax.rsqrt(squares / D + EPSILON)

    def squares_of(values):
        return jnp.sum(values * values, axis=1, keepdims=True)

    def normalize(buffer, row):
        squares = jnp.zeros((TOK, 1), F32)
        for j in range(SLOTS):
            squares = squares + squares_of(buffer[j].astype(F32))
        scale = scale_of(squares)
        for j in range(SLOTS):
            values = buffer[j].astype(F32) * scale * gains[row : row + 1, j * SLICE : (j + 1) * SLICE]
            normed[:, j * SLICE : (j + 1) * SLICE] = values.astype(BF16)

    def settle(current, branch, row, weight, result):
        squares = jnp.zeros((TOK, 1), F32)
        for j in range(SLOTS):
            squares = squares + squares_of(branch[j].astype(F32))
        scale = scale_of(squares)
        for j in range(SLOTS):
            step = branch[j].astype(F32) * scale * gains[row : row + 1, j * SLICE : (j + 1) * SLICE]
            result[j] = (current[j].astype(F32) + weight * step).astype(BF16)

    def silu(v):
        return v / (1.0 + jnp.exp(-v))

    def gate_and_up():
        def block(i, _):
            columns = pl.ds(pl.multiple_of(i * 256, 256), 256)
            both = jnp.dot(normed[...], full0[:, columns], preferred_element_type=F32)
            value = silu(both[:, :128]) * both[:, 128:]
            hidden[:, pl.ds(pl.multiple_of(i * 128, 128), 128)] = value.astype(BF16)
            return 0

        lax.fori_loop(0, 5, block, 0)
        both = jnp.dot(normed[...], full0[:, 1280:1408], preferred_element_type=F32)
        value = silu(both) * pltpu.roll(both, 64, 1)
        lane = lax.broadcasted_iota(jnp.int32, value.shape, 1)
        hidden[:, 640:768] = jnp.where(lane < 64, value, 0.0).astype(BF16)

    def slot_rows(slot):
        return pl.ds(pl.multiple_of(slot * SLICE, SLICE), SLICE)

    def down_product(slot):
        return turned_dot(hidden[...], full0[slot_rows(slot), 1408:])

    pump(0.0)
    gather_x(act, stream, lambda step: pump((3.0, 6.0, 9.0)[step]))
    normalize(act, 0)
    here = max(t for kind, c, t in order if kind == "wait" and c.part[0] == 0)
    pump(here)
    gate_and_up()
    pump(here + 2.0)
    branch1[tp] = reduce_x(
        0, down_product, lambda step: pump(here + (2.5, 3.5, 4.5, 5.5, 8.0)[step])
    ).astype(BF16)
    gather_x(branch1, branch1.at[tp], lambda step: pump(here + (10.0, 14.5, 18.0)[step]))
    pump(1e9)
    settle(act, branch1, 1, 0.5, first)

    normalize(first, 2)
    mix_in = jnp.dot(normed[...], full1[:, : 3 * CHANNELS], preferred_element_type=F32)
    conv_input = mix_in[:, 2 * CHANNELS :] * mix_in[:, :CHANNELS]
    conv[8:] = conv_input
    halo_out[...] = conv_input[TOK - 8 :]
    halo = send(halo_out, halo_in, next_place)
    halo.wait_recv()
    conv[:8] = jnp.where(fs == 0, 0.0, halo_in[...])
    mixed = taps[0:1, :] * conv[6 : 6 + TOK]
    for tap in range(1, TAPS):
        mixed = mixed + taps[tap : tap + 1, :] * conv[6 + tap : 6 + tap + TOK]
    hidden[:, :CHANNELS] = (mix_in[:, CHANNELS : 2 * CHANNELS] * mixed).astype(BF16)

    def out_product(slot):
        return turned_dot(hidden[:, :CHANNELS], full1[slot_rows(slot), 3 * CHANNELS :])

    branch2[tp] = reduce_x(1, out_product).astype(BF16)
    gather_x(branch2, branch2.at[tp])
    settle(first, branch2, 3, 1.0, second)

    normalize(second, 4)
    gate_and_up()
    branch = reduce_x(2, down_product)
    squares = jnp.broadcast_to(squares_of(branch), (TOK, 128))
    sq_out[...] = jnp.transpose(squares)[:8]
    got = [send(sq_out, sq_in.at[i], device) for i, device in enumerate(others)]
    total = sq_out[...]
    for copy in got:
        copy.wait_recv()
    for i in range(SLOTS - 1):
        total = total + sq_in[i]
    scale = jnp.transpose(scale_of(jnp.concatenate([total] * 16, axis=0)))[:, :1]
    step = branch * scale * gains[5:6, pl.ds(pl.multiple_of(tp * SLICE, SLICE), SLICE)]
    out[...] = (second[tp].astype(F32) + 0.5 * step).astype(BF16)

    for copy in copies:
        remote(copy).wait_send()
    for copy in sent:
        copy.wait_send()


def whole_layer(*arrays):
    order, copies = planned()

    def kernel(*refs):
        layer_kernel(order, copies, refs)

    slots = (SLOTS, TOK, SLICE)
    half = TOK // 2
    scratch = [pltpu.VMEM((ROWS * Z_LO * Y, w), BF16) for w in WIDTHS]
    scratch += [pltpu.SemaphoreType.DMA((len(copies),))] * 2
    scratch += [pltpu.SemaphoreType.DMA((X_COPIES,))] * 2
    scratch += [pltpu.VMEM(slots, BF16)] * 5
    scratch += [
        pltpu.VMEM((TOK, D), BF16),
        pltpu.VMEM((TOK, 768), BF16),
        pltpu.VMEM((4, TOK, SLICE), F32),
        pltpu.VMEM((3, 4, TOK, SLICE), BF16),
        pltpu.VMEM((3, 4, TOK, SLICE), BF16),
        pltpu.VMEM((3, 2, half, SLICE), BF16),
        pltpu.VMEM((3, 2, half, SLICE), BF16),
        pltpu.VMEM((3, 2, TOK, SLICE), BF16),
        pltpu.VMEM((3, 2, TOK, SLICE), BF16),
        pltpu.VMEM((TOK + 8, CHANNELS), F32),
        pltpu.VMEM((8, CHANNELS), F32),
        pltpu.VMEM((8, CHANNELS), F32),
        pltpu.VMEM((8, TOK), F32),
        pltpu.VMEM((SLOTS - 1, 8, TOK), F32),
    ]
    return pl.pallas_call(
        kernel,
        out_shape=jax.ShapeDtypeStruct(arrays[0].shape, BF16),
        in_specs=[pl.BlockSpec(memory_space=pltpu.VMEM)] * len(arrays),
        out_specs=pl.BlockSpec(memory_space=pltpu.VMEM),
        scratch_shapes=scratch,
        compiler_params=pltpu.CompilerParams(
            collective_id=0, has_side_effects=True, vmem_limit_bytes=60 * 2**20
        ),
    )(*arrays)


def shards(stream, norm_gains, w_gate, w_up, w_down, w_inner, w_bgate, w_cgate, conv_taps, w_out):
    return whole_layer(
        stream, norm_gains, w_gate, w_up, w_down.T, w_inner, w_bgate, w_cgate, w_out.T, conv_taps
    )


def solution(mesh):
    return jax.shard_map(
        shards,
        mesh=mesh,
        in_specs=(
            P(("rep", "fs"), "tp"),
            P(),
            P("fs", "tp"),
            P("fs", "tp"),
            P("tp", "fs"),
            P("fs", "tp"),
            P("fs", "tp"),
            P("fs", "tp"),
            P(None, "tp"),
            P("tp", "fs"),
        ),
        out_specs=P(("rep", "fs"), "tp"),
        check_vma=False,
    )
```

```python
import jax
import jax.numpy as jnp
from jax import lax
from jax.experimental import pallas as pl
from jax.experimental.pallas import tpu as pltpu
from jax.sharding import PartitionSpec as P

TAPS = 3
EPSILON = 1e-06
Z_LO, Z_ALL, Y = 8, 16, 4
ROWS = 64
PARTS = (
    ((0, 896, "y"), (896, 1280, "z")),
    ((0, 128, "y"), (128, 384, "z")),
)
WIDTHS = (2176, 512)
RATE = 52e3
HOP = 2.8
AHEAD = (2.5, 2.5)
LATER = 8
X_COPIES = 13 * 3 + 10 * 3 + 8


class Copy:
    def __init__(self, number, part, link, dz, dy, row, rows, after):
        self.number, self.part, self.link = number, part, link
        self.dz, self.dy, self.row, self.rows = dz, dy, row, rows
        self.after, self.tail = after, 0.0
        stream, index = part
        self.time = rows * PARTS[stream][index][1] * 2 / RATE
        self.start = None


def all_copies():
    copies = []

    def add(part, link, dz, dy, after, row=0, rows=ROWS):
        copies.append(Copy(len(copies), part, link, dz, dy, row, rows, list(after)))
        return copies[-1]

    half = ROWS // 2
    for stream, parts in enumerate(PARTS):
        for index, (_, _, first) in enumerate(parts):
            part = (stream, index)

            def along_z(dy, own):
                came = {0: own}
                for sign, link, row in ((-1, "z+", 0), (1, "z-", half)):
                    previous = own
                    for step in range(3):
                        previous = [add(part, link, sign * step, dy, previous)]
                        came[sign * (step + 1)] = previous
                    last = add(part, link, sign * 3, dy, previous, row, half)
                    came.setdefault(4, []).append(last)
                return came

            def along_y(dz, own):
                up = add(part, "y+", dz, 0, own)
                down = add(part, "y-", dz, 0, own)
                far = [
                    add(part, "y+", dz, -1, [up], 0, half),
                    add(part, "y-", dz, 1, [down], half, half),
                ]
                return {0: own, -1: [up], 1: [down], 2: far}

            if first == "y":
                for dy, got in along_y(0, []).items():
                    along_z(dy, got)
            else:
                for dz, got in along_z(0, []).items():
                    along_y(dz, got)
    for copy in reversed(copies):
        for before in copy.after:
            before.tail = max(before.tail, copy.tail + copy.time + HOP)
    return copies


def planned():
    copies = all_copies()
    free = dict.fromkeys(("y+", "y-", "z+", "z-"), 0.0)
    waiting, flying, here, order, now = list(copies), [], set(), [], 0.0
    while waiting or flying:
        ready = [c for c in waiting if all(b.number in here for b in c.after)]
        ready.sort(key=lambda c: (c.part[0], -c.tail, c.number))
        for copy in ready:
            if copy.part[0] and sum(c.part[0] == 0 for c in waiting) > LATER:
                break
            if free[copy.link] < now + AHEAD[copy.part[0]]:
                free[copy.link] = max(free[copy.link], now) + copy.time
                flying.append((free[copy.link] + HOP, copy.number, copy))
                waiting.remove(copy)
                order.append(("start", copy, now))
        flying.sort(key=lambda f: f[:2])
        now, _, copy = flying.pop(0)
        here.add(copy.number)
        order.append(("wait", copy, now))
    return order, copies


MESH = pl.DeviceIdType.MESH
TOK, D, SLOTS, SLICE = 256, 2048, 8, 256
UNITS, CHANNELS = 704, 128
F32, BF16 = jnp.float32, jnp.bfloat16


def turned_dot(x, turned):
    return lax.dot_general(x, turned, (((1,), (1,)), ((), ())), preferred_element_type=F32)


def layer_kernel(order, copies, refs):
    (stream, gains, w_gate, w_up, w_down, w_inner, w_bgate, w_cgate, w_out, taps, out, full0, full1,
     send_sem, recv_sem, x_send, x_recv, act, first, second, branch1, branch2, normed, hidden, acc,
     pair_out, pair_in, far_out, far_in, near_out, near_in, conv, halo_out, halo_in, sq_out,
     sq_in) = refs
    full = (full0, full1)
    rep, fs, tp = lax.axis_index("rep"), lax.axis_index("fs"), lax.axis_index("tp")
    z_lo, y = fs // Y, lax.rem(fs, Y)
    z = rep * Z_LO + z_lo
    x, core = tp // 2, lax.rem(tp, 2)

    def at(z_to, y_to):
        return (z_to // Z_LO, lax.rem(z_to, Z_LO) * Y + y_to, tp)

    def peer(slot):
        return (rep, fs, slot)

    def slot_of(dx, dc=0):
        return lax.rem(x + dx, 4) * 2 + (core if dc == 0 else 1 - core)

    place = {
        "y+": at(z, lax.rem(y + 1, Y)),
        "y-": at(z, lax.rem(y + Y - 1, Y)),
        "z+": at(lax.rem(z + 1, Z_ALL), y),
        "z-": at(lax.rem(z + Z_ALL - 1, Z_ALL), y),
    }
    up, down, partner = peer(slot_of(1)), peer(slot_of(3)), peer(slot_of(0, 1))
    after = (z * Y + y + 1 + Z_ALL * Y) % (Z_ALL * Y)
    next_place = at(after // Y, lax.rem(after, Y))
    others = [peer(lax.rem(tp + i, SLOTS)) for i in range(1, SLOTS)]

    barrier = pltpu.get_barrier_semaphore()
    greeted = [*place.values(), *others]
    for device in greeted:
        pl.semaphore_signal(barrier, inc=1, device_id=device, device_id_type=MESH)
    mine = pl.ds(pl.multiple_of(fs * ROWS, ROWS), ROWS)
    for i in range(5):
        columns = slice(128 * i, 128 * i + 128)
        full0[mine, 256 * i : 256 * i + 128] = w_gate[:, columns]
        full0[mine, 256 * i + 128 : 256 * i + 256] = w_up[:, columns]
    full0[mine, 1280:1408] = jnp.concatenate([w_gate[:, 640:], w_up[:, 640:]], axis=1)
    full0[mine, 1408:2048] = w_down[:, :640]
    rest = jnp.concatenate([w_down[:, 640:], jnp.zeros((ROWS, 64), BF16)], axis=1)
    full0[mine, 2048:2176] = rest
    full1[mine, :128] = w_inner[...]
    full1[mine, 128:256] = w_bgate[...]
    full1[mine, 256:384] = w_cgate[...]
    full1[mine, 384:] = w_out[...]
    act[tp] = stream[...]

    pl.semaphore_wait(barrier, len(greeted))

    def remote(copy):
        stream_, index = copy.part
        column, width, _ = PARTS[stream_][index]
        columns = pl.ds(column, width)
        block = lax.rem(z_lo + copy.dz + Z_LO, Z_LO) * Y + lax.rem(y + copy.dy + Y, Y)
        rows = pl.ds(pl.multiple_of(block * ROWS, ROWS) + copy.row, copy.rows)
        target = full[stream_].at[rows, columns]
        return pltpu.make_async_remote_copy(
            src_ref=target,
            dst_ref=target,
            send_sem=send_sem.at[copy.number],
            recv_sem=recv_sem.at[copy.number],
            device_id=place[copy.link],
            device_id_type=MESH,
        )

    events = list(order)

    def pump(until):
        while events and events[0][2] <= until:
            kind, copy, _ = events.pop(0)
            if kind == "start":
                remote(copy).start()
            else:
                remote(copy).wait_recv()

    sent = []

    def send(source, target, device):
        number = len(sent)
        copy = pltpu.make_async_remote_copy(
            src_ref=source,
            dst_ref=target,
            send_sem=x_send.at[number],
            recv_sem=x_recv.at[number],
            device_id=device,
            device_id_type=MESH,
        )
        copy.start()
        sent.append(copy)
        return copy

    def gather_x(buffer, source, pace=lambda step: None):
        half = TOK // 2
        low, high = pl.ds(0, half), pl.ds(half, half)
        mine, left, right, far = slot_of(0), slot_of(3), slot_of(1), slot_of(2)

        def same(ref, device):
            return send(ref, ref, device)

        near = {}
        for rows_up, rows_down in ((low, high), (high, low)):
            for key, rows, device in (("left", rows_up, up), ("right", rows_down, down)):
                near.setdefault(key, []).append(
                    send(source.at[rows], buffer.at[mine, rows], device)
                )
        pairs = [send(source, buffer.at[mine], partner)]
        pace(0)
        near["left"][0].wait_recv()
        far_low = same(buffer.at[left, low], up)
        pairs.append(same(buffer.at[left, low], partner))
        near["right"][0].wait_recv()
        far_high = same(buffer.at[right, high], down)
        pairs.append(same(buffer.at[right, high], partner))
        near["left"][1].wait_recv()
        pairs.append(same(buffer.at[left, high], partner))
        near["right"][1].wait_recv()
        pairs.append(same(buffer.at[right, low], partner))
        pace(1)
        far_low.wait_recv()
        pairs.append(same(buffer.at[far, low], partner))
        far_high.wait_recv()
        pairs.append(same(buffer.at[far, high], partner))
        pace(2)
        for copy in pairs:
            copy.wait_recv()

    def reduce_x(use, product, pace=lambda step: None):
        half = TOK // 2
        low, high = pl.ds(0, half), pl.ds(half, half)
        pair = {}

        def give(d):
            pair_out[use, d] = product(slot_of(d, 1)).astype(BF16)
            pair[d] = send(pair_out.at[use, d], pair_in.at[use, d], partner)

        def chip_sum(d, rows):
            return acc[d, rows] + pair_in[use, d, rows].astype(F32)

        give(2)
        acc[2] = product(slot_of(2))
        give(1)
        give(3)
        give(0)
        pace(0)
        pair[2].wait_recv()
        far_out[use, 0] = chip_sum(2, low).astype(BF16)
        far_low = send(far_out.at[use, 0], far_in.at[use, 0], up)
        far_out[use, 1] = chip_sum(2, high).astype(BF16)
        far_high = send(far_out.at[use, 1], far_in.at[use, 1], down)
        pace(1)
        acc[1] = product(slot_of(1))
        pair[1].wait_recv()
        near_out[use, 0, high] = chip_sum(1, high).astype(BF16)
        near = [send(near_out.at[use, 0, high], near_in.at[use, 0, high], up)]
        acc[3] = product(slot_of(3))
        pair[3].wait_recv()
        near_out[use, 1, low] = chip_sum(3, low).astype(BF16)
        near.append(send(near_out.at[use, 1, low], near_in.at[use, 1, low], down))
        acc[0] = product(slot_of(0))
        pace(2)
        pair[0].wait_recv()
        pace(3)
        far_low.wait_recv()
        near_out[use, 0, low] = (chip_sum(1, low) + far_in[use, 0].astype(F32)).astype(BF16)
        near.append(send(near_out.at[use, 0, low], near_in.at[use, 0, low], up))
        far_high.wait_recv()
        near_out[use, 1, high] = (chip_sum(3, high) + far_in[use, 1].astype(F32)).astype(BF16)
        near.append(send(near_out.at[use, 1, high], near_in.at[use, 1, high], down))
        pace(4)
        for copy in near:
            copy.wait_recv()
        total = acc[0] + pair_in[use, 0].astype(F32)
        return total + near_in[use, 0].astype(F32) + near_in[use, 1].astype(F32)

    def scale_of(squares):
        return lax.rsqrt(squares / D + EPSILON)

    def squares_of(values):
        return jnp.sum(values * values, axis=1, keepdims=True)

    def normalize(buffer, row):
        squares = jnp.zeros((TOK, 1), F32)
        for j in range(SLOTS):
            squares = squares + squares_of(buffer[j].astype(F32))
        scale = scale_of(squares)
        for j in range(SLOTS):
            values = buffer[j].astype(F32) * scale * gains[row : row + 1, j * SLICE : (j + 1) * SLICE]
            normed[:, j * SLICE : (j + 1) * SLICE] = values.astype(BF16)

    def settle(current, branch, row, weight, result):
        squares = jnp.zeros((TOK, 1), F32)
        for j in range(SLOTS):
            squares = squares + squares_of(branch[j].astype(F32))
        scale = scale_of(squares)
        for j in range(SLOTS):
            step = branch[j].astype(F32) * scale * gains[row : row + 1, j * SLICE : (j + 1) * SLICE]
            result[j] = (current[j].astype(F32) + weight * step).astype(BF16)

    def silu(v):
        return v / (1.0 + jnp.exp(-v))

    def gate_and_up():
        def block(i, _):
            columns = pl.ds(pl.multiple_of(i * 256, 256), 256)
            both = jnp.dot(normed[...], full0[:, columns], preferred_element_type=F32)
            value = silu(both[:, :128]) * both[:, 128:]
            hidden[:, pl.ds(pl.multiple_of(i * 128, 128), 128)] = value.astype(BF16)
            return 0

        lax.fori_loop(0, 5, block, 0)
        both = jnp.dot(normed[...], full0[:, 1280:1408], preferred_element_type=F32)
        value = silu(both) * pltpu.roll(both, 64, 1)
        lane = lax.broadcasted_iota(jnp.int32, value.shape, 1)
        hidden[:, 640:768] = jnp.where(lane < 64, value, 0.0).astype(BF16)

    def slot_rows(slot):
        return pl.ds(pl.multiple_of(slot * SLICE, SLICE), SLICE)

    def down_product(slot):
        return turned_dot(hidden[...], full0[slot_rows(slot), 1408:])

    pump(0.0)
    gather_x(act, stream, lambda step: pump((3.0, 6.0, 9.0)[step]))
    normalize(act, 0)
    here = max(t for kind, c, t in order if kind == "wait" and c.part[0] == 0)
    pump(here)
    gate_and_up()
    pump(here + 2.0)
    branch1[tp] = reduce_x(
        0, down_product, lambda step: pump(here + (2.5, 3.5, 4.5, 5.5, 8.0)[step])
    ).astype(BF16)
    gather_x(branch1, branch1.at[tp], lambda step: pump(here + (10.0, 14.5, 18.0)[step]))
    pump(1e9)
    settle(act, branch1, 1, 0.5, first)

    normalize(first, 2)
    mix_in = jnp.dot(normed[...], full1[:, : 3 * CHANNELS], preferred_element_type=F32)
    conv_input = mix_in[:, 2 * CHANNELS :] * mix_in[:, :CHANNELS]
    conv[8:] = conv_input
    halo_out[...] = conv_input[TOK - 8 :]
    halo = send(halo_out, halo_in, next_place)
    halo.wait_recv()
    conv[:8] = jnp.where(fs == 0, 0.0, halo_in[...])
    mixed = taps[0:1, :] * conv[6 : 6 + TOK]
    for tap in range(1, TAPS):
        mixed = mixed + taps[tap : tap + 1, :] * conv[6 + tap : 6 + tap + TOK]
    hidden[:, :CHANNELS] = (mix_in[:, CHANNELS : 2 * CHANNELS] * mixed).astype(BF16)

    def out_product(slot):
        return turned_dot(hidden[:, :CHANNELS], full1[slot_rows(slot), 3 * CHANNELS :])

    branch2[tp] = reduce_x(1, out_product).astype(BF16)
    gather_x(branch2, branch2.at[tp])
    settle(first, branch2, 3, 1.0, second)

    normalize(second, 4)
    gate_and_up()
    branch = reduce_x(2, down_product)
    squares = jnp.broadcast_to(squares_of(branch), (TOK, 128))
    sq_out[...] = jnp.transpose(squares)[:8]
    got = [send(sq_out, sq_in.at[i], device) for i, device in enumerate(others)]
    total = sq_out[...]
    for copy in got:
        copy.wait_recv()
    for i in range(SLOTS - 1):
        total = total + sq_in[i]
    scale = jnp.transpose(scale_of(jnp.concatenate([total] * 16, axis=0)))[:, :1]
    step = branch * scale * gains[5:6, pl.ds(pl.multiple_of(tp * SLICE, SLICE), SLICE)]
    out[...] = (second[tp].astype(F32) + 0.5 * step).astype(BF16)

    for copy in copies:
        remote(copy).wait_send()
    for copy in sent:
        copy.wait_send()


def whole_layer(*arrays):
    order, copies = planned()

    def kernel(*refs):
        layer_kernel(order, copies, refs)

    slots = (SLOTS, TOK, SLICE)
    half = TOK // 2
    scratch = [pltpu.VMEM((ROWS * Z_LO * Y, w), BF16) for w in WIDTHS]
    scratch += [pltpu.SemaphoreType.DMA((len(copies),))] * 2
    scratch += [pltpu.SemaphoreType.DMA((X_COPIES,))] * 2
    scratch += [pltpu.VMEM(slots, BF16)] * 5
    scratch += [
        pltpu.VMEM((TOK, D), BF16),
        pltpu.VMEM((TOK, 768), BF16),
        pltpu.VMEM((4, TOK, SLICE), F32),
        pltpu.VMEM((3, 4, TOK, SLICE), BF16),
        pltpu.VMEM((3, 4, TOK, SLICE), BF16),
        pltpu.VMEM((3, 2, half, SLICE), BF16),
        pltpu.VMEM((3, 2, half, SLICE), BF16),
        pltpu.VMEM((3, 2, TOK, SLICE), BF16),
        pltpu.VMEM((3, 2, TOK, SLICE), BF16),
        pltpu.VMEM((TOK + 8, CHANNELS), F32),
        pltpu.VMEM((8, CHANNELS), F32),
        pltpu.VMEM((8, CHANNELS), F32),
        pltpu.VMEM((8, TOK), F32),
        pltpu.VMEM((SLOTS - 1, 8, TOK), F32),
    ]
    return pl.pallas_call(
        kernel,
        out_shape=jax.ShapeDtypeStruct(arrays[0].shape, BF16),
        in_specs=[pl.BlockSpec(memory_space=pltpu.VMEM)] * len(arrays),
        out_specs=pl.BlockSpec(memory_space=pltpu.VMEM),
        scratch_shapes=scratch,
        compiler_params=pltpu.CompilerParams(
            collective_id=0, has_side_effects=True, vmem_limit_bytes=60 * 2**20
        ),
    )(*arrays)


def shards(stream, norm_gains, w_gate, w_up, w_down, w_inner, w_bgate, w_cgate, conv_taps, w_out):
    return whole_layer(
        stream, norm_gains, w_gate, w_up, w_down.T, w_inner, w_bgate, w_cgate, w_out.T, conv_taps
    )


def solution(mesh):
    return jax.shard_map(
        shards,
        mesh=mesh,
        in_specs=(
            P(("rep", "fs"), "tp"),
            P(),
            P("fs", "tp"),
            P("fs", "tp"),
            P("tp", "fs"),
            P("fs", "tp"),
            P("fs", "tp"),
            P("fs", "tp"),
            P(None, "tp"),
            P("tp", "fs"),
        ),
        out_specs=P(("rep", "fs"), "tp"),
        check_vma=False,
    )
```
